32 devices in a mesh: sp: 8 (over z, x), tp: 4 (over y, core).
Axes of the slice: x: 2, y: 2, z: 4, core: 2. Of those that a mesh axis runs over, the one named last changes fastest.
Arguments:
- residual: bfloat16 [1024, 2048], P('sp'), may hold values from -6 to 6
- queries: bfloat16 [1024, 2048], P('sp', 'tp'), may hold values from -6 to 6
- keys: bfloat16 [1024, 2048], P('sp', 'tp'), may hold values from -6 to 6
- values: bfloat16 [1024, 2048], P('sp', 'tp'), may hold values from -24 to 24
- stick_bias: bfloat16 [32, 1024], P('tp', 'sp'), may hold values from 2 to 13
- query_gain: float32 [64], replicated, may hold values from 0.1 to 1.9
- key_gain: float32 [64], replicated, may hold values from 0.1 to 1.9
- out_weight: bfloat16 [2048, 2048], P('tp'), may hold values from -0.25 to 0.25
- norm_gain: float32 [2048], replicated, may hold values from 0.1 to 1.9
- route_ids: int32 [1024, 2], P('sp'), may hold values from 0 to 7, all different within a row; in each aligned block of 128 rows (0 to 127, 128 to 255, ...) at most 40 rows name the same one
- route_weights: float32 [1024, 2], P('sp'), may hold values from 0.1 to 1
- gate_weight: bfloat16 [8, 2048, 2048], P('sp', None, 'tp'), may hold values from -3 to 3
- up_weight: bfloat16 [8, 2048, 2048], P('sp', None, 'tp'), may hold values from -3 to 3
- down_weight: bfloat16 [8, 2048, 2048], P('sp', 'tp'), may hold values from -0.125 to 0.125
Outputs:
- layer_out: bfloat16 [1024, 2048], P('sp', 'tp')
The draws below stay inside these ranges and needn't reach their ends.
Inputs may be any that keep to these rules, and one draw needn't show every extreme that they name: `route_ids`: each row names 2 different experts. In every aligned block of 128 rows at most 40 rows name one expert, and in every draw some expert is named by exactly 40 rows of some block.
All inputs are finite; a program needn't handle non-finite values.
Results may differ from the reference program's by a relative error of at most 0.028.
Values may be sent and summed in bfloat16 or wider, within the bound.
A program may use at most 64 MiB of HBM per device.

```python
import math
import jax
import jax.numpy as jnp
import numpy as np
from jax import lax

D = 2048
HEADS = 32
HD = 64
FF = 2048
TOP_K = 2
TOK_DEV = 128
TOKENS = 1024
EXPERTS = 8
CAP = 40
N_SP = 8
N_TP = 4


def draw_stick_bias(key, part):
    subkeys = jax.random.split(jax.random.fold_in(key, 13), 5)
    slow_share = 5
    slow_heads = jax.random.randint(subkeys[0], (HEADS, 1), 0, 10) < slow_share
    base_slow = math.log(float(TOKENS)) + jax.random.uniform(subkeys[1], (HEADS, 1), jnp.float32, -0.3, 0.5)
    base_fast = math.log(40.0) + jax.random.uniform(subkeys[2], (HEADS, 1), jnp.float32, -0.3, 0.3)
    drift = jnp.repeat(jax.random.uniform(subkeys[3], (HEADS, TOKENS // 32), jnp.float32, -0.7, 0.7), 32, axis=1)
    rough = jax.random.uniform(subkeys[4], (HEADS, TOKENS), jnp.float32, -0.5, 0.5)
    return (jnp.where(slow_heads, base_slow, base_fast) + drift + rough).astype(jnp.bfloat16)


def expert_matrix(key):
    first_key, second_key = jax.random.split(key)
    low_scale = 0.5
    high_scale = 3.0
    column_scale = jnp.exp(jax.random.uniform(second_key, (EXPERTS, 1, FF), jnp.float32, math.log(low_scale), math.log(high_scale)))
    entries = jax.random.truncated_normal(first_key, -4.0, 4.0, (EXPERTS, D, FF), jnp.float32)
    return jnp.clip(entries * D ** (-0.5) * column_scale, -3.0, 3.0).astype(jnp.bfloat16)


def draw_gate_weight(key, part):
    return expert_matrix(jax.random.fold_in(key, 11))


def draw_up_weight(key, part):
    return expert_matrix(jax.random.fold_in(key, 12))


def level_of(own_key, extent, pieces, low, top_value):
    def one(position, shards_of):
        steps = jax.random.uniform(jax.random.fold_in(jax.random.fold_in(own_key, 6), position), (shards_of,), jnp.float32, low / len(pieces), top_value / len(pieces))
        return jnp.repeat(jnp.exp(steps), extent[position] // shards_of).reshape((-1,) + (1,) * (len(extent) - position - 1))

    factor_of = one(*pieces[0])
    for cut in pieces[1:]:
        factor_of = factor_of * one(*cut)
    return factor_of


def deal_out(stream_key, own, number, rows, count, top, most, skew):
    ranking = jax.random.permutation(stream_key, count)
    crowded, ordinary = portions_of(count, rows * top, most, skew, True), portions_of(count, rows * top, most, skew, False)
    places = jnp.arange(count)

    def named(sizes, rotation):
        used = int((sizes > 0).sum())
        fixed = max(1, used // 4)
        moved = fixed + (places - fixed + rotation * (used - fixed)) % max(1, count - fixed)
        return jnp.zeros((count,), jnp.int32).at[ranking[jnp.where(places < fixed, places, moved)]].set(jnp.asarray(sizes, jnp.int32))

    sizes = jnp.where(number % 4 == 0, named(crowded, number // 4), named(ordinary, number - number // 4 - 1))
    mixed = jax.random.permutation(jax.random.fold_in(own, 3), count)
    source_of, receiver = mixed[0:count // 2 * 2:2], mixed[1:count // 2 * 2:2]
    slack = jnp.minimum(sizes[source_of] - 1, most - sizes[receiver]) // 2
    slack = jnp.where((source_of == ranking[0]) | (receiver == ranking[0]) | (sizes[receiver] == 0), 0, jnp.maximum(slack, 0))
    moved = jax.random.randint(jax.random.fold_in(own, 4), (count // 2,), 0, 1 << 20) % (slack + 1)
    sizes = sizes.at[source_of].add(-moved).at[receiver].add(moved)
    items = jnp.searchsorted(jnp.cumsum(sizes), jnp.arange(rows * top), side="right").astype(jnp.int32)
    table = items.reshape(top, rows).T
    table = table[jax.random.permutation(jax.random.fold_in(own, 1), rows)]
    rotation = jax.random.randint(jax.random.fold_in(own, 2), (rows, 1), 0, top)
    return jnp.take_along_axis(table, (jnp.arange(top)[None, :] + rotation) % top, axis=1)


def portions_of(amount, total, reach, lean, full):
    loads = [(1 << 20) // math.isqrt(rank ** lean) + 1 for rank in range(1, amount + 1)]
    largest = reach if full else min(reach, max(-(-total // amount), total * loads[0] // sum(loads)))
    least = 1 if total - largest >= amount - 1 else 0
    counts, spare = [largest] + [least] * (amount - 1), total - largest - least * (amount - 1)
    while spare > 0:
        free = [i for i in range(1, amount) if counts[i] < largest] or [i for i in range(1, amount) if counts[i] < reach]
        whole, budget = sum([loads[i] for i in free]), spare
        for i in free:
            more = min(reach - counts[i], max(1, budget * loads[i] // whole), spare)
            counts[i] = counts[i] + more
            spare = spare - more
    return np.array(counts)


def scatter_about(rng, dims, deviation, bound, cuts=(), held_as=jnp.bfloat16):
    loudness = level_of(rng, dims, cuts, -0.22, 0.18) if cuts else 1.0
    values = jax.random.normal(rng, dims, jnp.float32) * deviation * loudness
    return jnp.minimum(jnp.maximum(values, -bound), bound).astype(held_as)


def setup_inputs(seed: int = 0) -> dict:
    splits = jax.random.split(jax.random.key(seed), 15)
    residual = scatter_about(splits[0], (TOKENS, D), 1.0, 6.0, ((0, 8),))
    queries = scatter_about(splits[1], (TOKENS, HEADS * HD), 1.0, 6.0, ((0, 8), (1, 4)))
    keys = scatter_about(splits[2], (TOKENS, HEADS * HD), 1.0, 6.0, ((0, 8), (1, 4)))
    values = scatter_about(splits[3], (TOKENS, HEADS * HD), 4.0, 24.0, ((0, 8), (1, 4)))
    stick_bias = draw_stick_bias(jax.random.fold_in(splits[14], 71), 0)
    query_gain = jnp.clip(1.0 + 0.18 * jax.random.normal(splits[5], (HD,), jnp.float32), 0.1, 1.9)
    key_gain = jnp.clip(1.0 + 0.18 * jax.random.normal(splits[6], (HD,), jnp.float32), 0.1, 1.9)
    out_weight = scatter_about(splits[7], (HEADS * HD, D), (D // 4) ** -0.5, 0.25, ((0, 4),))
    norm_gain = jnp.clip(1.0 + 0.18 * jax.random.normal(splits[8], (D,), jnp.float32), 0.1, 1.9)
    route_ids_keys = jax.random.split(jax.random.fold_in(splits[9], 1), TOKENS // TOK_DEV)
    route_ids_turns = jax.random.permutation(jax.random.fold_in(splits[9], 3), TOKENS // TOK_DEV)
    route_ids = jax.vmap(lambda own, number: deal_out(jax.random.fold_in(splits[9], 2), own, number, TOK_DEV, EXPERTS, TOP_K, CAP, 1))(route_ids_keys, route_ids_turns).reshape((TOKENS, TOP_K))
    route_weights = jnp.clip(jnp.exp(math.log(1.0) - 2.3025851 * jax.random.uniform(splits[10], (TOKENS, TOP_K), jnp.float32) ** level_of(splits[10], (TOKENS, TOP_K), ((0, 8),), -0.2, 0.2)), 0.1, 1.0)
    gate_weight = draw_gate_weight(jax.random.fold_in(splits[14], 71), 0)
    up_weight = draw_up_weight(jax.random.fold_in(splits[14], 71), 0)
    down_weight = scatter_about(splits[13], (EXPERTS, FF, D), FF ** -0.5, 0.125, ((0, 8), (1, 4)))
    return {"residual": residual, "queries": queries, "keys": keys, "values": values, "stick_bias": stick_bias, "query_gain": query_gain, "key_gain": key_gain, "out_weight": out_weight, "norm_gain": norm_gain, "route_ids": route_ids, "route_weights": route_weights, "gate_weight": gate_weight, "up_weight": up_weight, "down_weight": down_weight}


epsilon = 1e-06
clamp_limit = 7.0
swish_scale = 1.702

def head_normalize(packed, gain):
    values_f = packed.astype(jnp.float32).reshape(packed.shape[0], -1, gain.shape[0])
    scaled = values_f * lax.rsqrt(lax.optimization_barrier(jnp.mean(values_f * values_f, axis=-1, keepdims=True)) + epsilon) * gain
    return scaled.astype(jnp.bfloat16)

def activate(gate_pre, up_pre):
    gate_top = jnp.minimum(gate_pre, clamp_limit)
    up_clip = jnp.clip(up_pre, -clamp_limit, clamp_limit)
    return (up_clip + 1.0) * (gate_top * jax.nn.sigmoid(swish_scale * gate_top))

def slot_table(picked, expert_count, capacity):
    flat_ids = picked.reshape(-1)
    one_hot = (flat_ids[:, None] == jnp.arange(expert_count, dtype=jnp.int32)[None, :]).astype(jnp.int32)
    before = lax.optimization_barrier(jnp.sum((jnp.cumsum(one_hot, axis=0) - one_hot) * one_hot, axis=1))
    return (flat_ids * capacity + before).astype(jnp.int32)

def attend_head(inputs):
    query_head, key_head, value_head, bias_head = inputs
    block_len = math.gcd(TOKENS, 512)
    positions = jnp.arange(TOKENS, dtype=jnp.int32)
    bias_row = bias_head.astype(jnp.float32)[None, :]

    def attend_block(first_row):
        query_block = lax.dynamic_slice_in_dim(query_head, first_row, block_len, 0)
        scores = jnp.dot(query_block, key_head.T, preferred_element_type=jnp.float32) * HD ** (-0.5) - bias_row
        query_pos = first_row + jnp.arange(block_len, dtype=jnp.int32)
        causal = positions[None, :] < query_pos[:, None]
        log_stay = jnp.where(causal, jax.nn.log_sigmoid(-scores), 0.0)
        later_sum = lax.cumsum(log_stay, axis=1, reverse=True) - log_stay
        weight = jnp.where(causal, jnp.exp(jax.nn.log_sigmoid(scores) + later_sum), 0.0).astype(jnp.bfloat16)
        return jnp.dot(weight, value_head, preferred_element_type=jnp.float32).astype(jnp.bfloat16)
    firsts = jnp.arange(TOKENS // block_len, dtype=jnp.int32) * block_len
    return lax.map(attend_block, firsts).reshape(TOKENS, HD)

def run_expert(inputs):
    routed_rows, gate_mat, up_mat, down_mat = inputs
    gate_pre = jnp.dot(routed_rows, gate_mat, preferred_element_type=jnp.float32)
    up_pre = jnp.dot(routed_rows, up_mat, preferred_element_type=jnp.float32)
    hidden = activate(gate_pre, up_pre).astype(jnp.bfloat16)
    group = FF // N_TP
    partial_value = jnp.einsum('rtf,tfd->trd', hidden.reshape(-1, N_TP, group).astype(jnp.float32), down_mat.reshape(N_TP, group, D).astype(jnp.float32))
    partial_value = lax.optimization_barrier(partial_value.astype(jnp.bfloat16))
    return lax.optimization_barrier(jnp.sum(partial_value.astype(jnp.float32), axis=0)).astype(jnp.bfloat16)

def block_sources(slot_index):
    tok_index = jnp.arange(TOK_DEV * TOP_K, dtype=jnp.int32) // TOP_K
    return jnp.zeros((EXPERTS * CAP,), jnp.int32).at[slot_index].set(tok_index)

def block_filled(slot_index):
    return jnp.zeros((EXPERTS * CAP,), jnp.bfloat16).at[slot_index].set(jnp.ones((TOK_DEV * TOP_K,), jnp.bfloat16))

def block_rows(normed_block, source_rows, filled_rows):
    return normed_block[source_rows] * filled_rows[:, None]

def block_take(back_block, slot_index):
    return back_block[slot_index]

def block_slots(picked):
    return slot_table(picked, EXPERTS, CAP)

def reference(residual, queries, keys, values, stick_bias, query_gain, key_gain, out_weight, norm_gain, route_ids, route_weights, gate_weight, up_weight, down_weight):
    query_normed = head_normalize(queries, query_gain).transpose(1, 0, 2)
    key_normed = head_normalize(keys, key_gain).transpose(1, 0, 2)
    value_heads = values.reshape(TOKENS, HEADS, HD).transpose(1, 0, 2)
    attended = lax.map(attend_head, (query_normed, key_normed, value_heads, stick_bias))
    attended = attended.transpose(1, 0, 2).reshape(TOKENS, HEADS * HD)
    group = HEADS * HD // N_TP
    mixed_sum = jnp.zeros((TOKENS, D), jnp.float32)
    for member in range(N_TP):
        partial_value = jnp.dot(attended[:, member * group:(member + 1) * group], out_weight[member * group:(member + 1) * group], preferred_element_type=jnp.float32)
        partial_value = lax.optimization_barrier(partial_value.astype(jnp.bfloat16))
        mixed_sum = mixed_sum + partial_value.astype(jnp.float32)
    after_mixer = (residual.astype(jnp.float32) + mixed_sum).astype(jnp.bfloat16)
    after_f = after_mixer.astype(jnp.float32)
    normed = (after_f * lax.rsqrt(lax.optimization_barrier(jnp.mean(after_f * after_f, axis=-1, keepdims=True)) + epsilon) * norm_gain).astype(jnp.bfloat16)
    slot_index = jax.vmap(block_slots)(route_ids.reshape(N_SP, TOK_DEV, TOP_K))
    source_rows = jax.vmap(block_sources)(slot_index)
    filled_rows = jax.vmap(block_filled)(slot_index)
    outgoing = jax.vmap(block_rows)(normed.reshape(N_SP, TOK_DEV, D), source_rows, filled_rows)
    incoming = outgoing.reshape(N_SP, EXPERTS, CAP, D).transpose(1, 0, 2, 3).reshape(EXPERTS, N_SP * CAP, D)
    results = lax.map(run_expert, (incoming, gate_weight, up_weight, down_weight))
    arrived = results.reshape(EXPERTS, N_SP, CAP, D).transpose(1, 0, 2, 3).reshape(N_SP, EXPERTS * CAP, D)
    taken_rows = jax.vmap(block_take)(arrived, slot_index).astype(jnp.float32).reshape(TOKENS, TOP_K, D)
    routed = lax.optimization_barrier(jnp.sum(taken_rows * route_weights[:, :, None], axis=1))
    return (after_f + routed).astype(jnp.bfloat16)
```

```python
import functools
import math

import jax
import jax.numpy as jnp
from jax import lax
from jax.experimental import pallas as pl
from jax.experimental.pallas import tpu as pltpu
from jax.sharding import PartitionSpec as P

epsilon = 1e-06
clamp_limit = 7.0
swish_scale = 1.702


def head_normalize(packed, gain):
    values_f = packed.astype(jnp.float32).reshape(packed.shape[0], -1, gain.shape[0])
    scaled = (
        values_f * lax.rsqrt(jnp.mean(values_f * values_f, axis=-1, keepdims=True) + epsilon) * gain
    )
    return scaled.astype(jnp.bfloat16)


def activate(gate_pre, up_pre):
    gate_top = jnp.minimum(gate_pre, clamp_limit)
    up_clip = jnp.clip(up_pre, -clamp_limit, clamp_limit)
    return (up_clip + 1.0) * (gate_top * jax.nn.sigmoid(swish_scale * gate_top))


def slot_table(picked, expert_count, capacity):
    flat_ids = picked.reshape(-1)
    one_hot = (flat_ids[:, None] == jnp.arange(expert_count, dtype=jnp.int32)[None, :]).astype(
        jnp.int32
    )
    before = jnp.sum((jnp.cumsum(one_hot, axis=0) - one_hot) * one_hot, axis=1)
    return flat_ids * capacity + before


def key_block(state_pair, queries_n, keys_block, values_block, bias_block, first_key, query_pos):
    summed, log_carry = state_pair
    key_count = bias_block.shape[1]
    head_total = bias_block.shape[0]
    keys_heads = keys_block.reshape(key_count, head_total, -1)
    values_heads = values_block.reshape(key_count, head_total, -1)
    head_dim = keys_heads.shape[2]
    scores = jnp.einsum(
        "qhd,khd->hqk", queries_n, keys_heads, preferred_element_type=jnp.float32
    ) * head_dim ** (-0.5)
    scores = scores - bias_block.astype(jnp.float32)[:, None, :]
    key_pos = first_key + jnp.arange(key_count, dtype=jnp.int32)
    causal = ((key_pos[None, :] < query_pos[:, None]) & (key_pos[None, :] >= 0))[None]
    log_stay = jnp.where(causal, jax.nn.log_sigmoid(-scores), 0.0)
    later_sum = lax.cumsum(log_stay, axis=2, reverse=True) - log_stay
    weight = jnp.where(
        causal, jnp.exp(jax.nn.log_sigmoid(scores) + later_sum + log_carry[:, :, None]), 0.0
    )
    summed = summed + jnp.einsum(
        "hqk,khd->qhd",
        weight.astype(jnp.bfloat16),
        values_heads,
        preferred_element_type=jnp.float32,
    )
    return (summed, log_carry + jnp.sum(log_stay, axis=2))


def per_device(
    residual,
    queries,
    keys,
    values,
    stick_bias,
    query_gain,
    key_gain,
    out_weight,
    norm_gain,
    route_ids,
    route_weights,
    gate_weight,
    up_weight,
    down_weight,
):
    tok_rows = queries.shape[0]
    width_sp = lax.axis_size("sp")
    offset = lax.axis_index("sp") * tok_rows
    query_pos = offset + jnp.arange(tok_rows, dtype=jnp.int32)
    queries_n = head_normalize(queries, query_gain)
    keys_n = head_normalize(keys, key_gain).reshape(tok_rows, -1)
    head_total = stick_bias.shape[0]
    head_dim = query_gain.shape[0]
    state_pair = (
        jnp.zeros((tok_rows, head_total, head_dim), jnp.float32),
        jnp.zeros((head_total, tok_rows), jnp.float32),
    )
    all_keys, all_values, all_bias = (
        lax.all_gather(keys_n, "sp", axis=0, tiled=True),
        lax.all_gather(values, "sp", axis=0, tiled=True),
        lax.all_gather(stick_bias, "sp", axis=1, tiled=True),
    )
    key_total = all_keys.shape[0]
    block_len = math.gcd(key_total, 512)
    block_total = key_total // block_len

    def sweep_block(block_step, running):
        first_key = (block_total - 1 - block_step) * block_len
        return key_block(
            running,
            queries_n,
            lax.dynamic_slice_in_dim(all_keys, first_key, block_len, 0),
            lax.dynamic_slice_in_dim(all_values, first_key, block_len, 0),
            lax.dynamic_slice_in_dim(all_bias, first_key, block_len, 1),
            first_key,
            query_pos,
        )

    state_pair = lax.fori_loop(0, block_total, sweep_block, state_pair)
    attended = state_pair[0].reshape(tok_rows, head_total * head_dim).astype(jnp.bfloat16)
    partial_value = jnp.dot(attended, out_weight, preferred_element_type=jnp.float32)
    model_width = residual.shape[1]
    expert_count = width_sp * gate_weight.shape[0]
    pick_count = route_ids.shape[1]
    capacity = (5 * tok_rows * pick_count + 4 * expert_count - 1) // (4 * expert_count)
    slot_index = slot_table(route_ids, expert_count, capacity)
    assigned = slot_index.shape[0]
    source = (
        jnp.zeros((expert_count * capacity,), jnp.int32)
        .at[slot_index]
        .set(jnp.arange(assigned, dtype=jnp.int32) // pick_count)
    )
    filled = (
        jnp.zeros((expert_count * capacity,), jnp.bfloat16)
        .at[slot_index]
        .set(jnp.ones((assigned,), jnp.bfloat16))
    )
    gate_local = gate_weight[0]
    up_local = up_weight[0]
    down_local = down_weight[0]
    mixed_share = lax.psum_scatter(
        partial_value.astype(jnp.bfloat16), "tp", scatter_dimension=1, tiled=True
    ).astype(jnp.float32)
    own_width = mixed_share.shape[1]
    col_start = lax.axis_index("tp") * own_width
    own_res = lax.dynamic_slice_in_dim(residual, col_start, own_width, 1).astype(jnp.float32)
    own_cols = (own_res + mixed_share).astype(jnp.bfloat16).astype(jnp.float32)
    square_total = lax.psum(jnp.sum(own_cols * own_cols, axis=1), "tp")
    gain_cols = lax.dynamic_slice_in_dim(norm_gain, col_start, own_width, 0)
    normed_share = (
        own_cols * lax.rsqrt(square_total / model_width + epsilon)[:, None] * gain_cols
    ).astype(jnp.bfloat16)
    outgoing = (normed_share[source] * filled[:, None]).reshape(expert_count, capacity, -1)
    piece = lax.all_gather(
        lax.all_to_all(outgoing, "sp", split_axis=0, concat_axis=0, tiled=True),
        "tp",
        axis=2,
        tiled=True,
    )
    gate_pre = jnp.einsum("scd,df->scf", piece, gate_local, preferred_element_type=jnp.float32)
    up_pre = jnp.einsum("scd,df->scf", piece, up_local, preferred_element_type=jnp.float32)
    hidden = activate(gate_pre, up_pre).astype(jnp.bfloat16)
    share = jnp.einsum("scf,fd->scd", hidden, down_local, preferred_element_type=jnp.float32)
    returned = lax.psum_scatter(share.astype(jnp.bfloat16), "tp", scatter_dimension=2, tiled=True)
    arrived = lax.all_to_all(returned, "sp", split_axis=0, concat_axis=0, tiled=True)
    columns = arrived.shape[2]
    taken_rows = arrived.reshape(expert_count * capacity, columns)[slot_index]
    taken_rows = taken_rows.astype(jnp.float32).reshape(tok_rows, pick_count, columns)
    routed = jnp.sum(taken_rows * route_weights[:, :, None], axis=1)
    return (own_cols + routed).astype(jnp.bfloat16)


f32 = jnp.float32
bf16 = jnp.bfloat16
MESH = pl.DeviceIdType.MESH


def fused_kernel(
    dims,
    q_ref,
    k_ref,
    v_ref,
    bias_ref,
    qg_ref,
    kg_ref,
    ng_ref,
    ids_ref,
    rw_ref,
    res_hbm,
    ow_hbm,
    gw_hbm,
    uw_hbm,
    dw_hbm,
    out_ref,
    res_v,
    ow_v,
    gw_v,
    uw_v,
    dw_v,
    pack_s,
    pack_r,
    kn_v,
    vn_v,
    att_s,
    att_r,
    mix_s,
    mix_r,
    mix_as,
    mix_ar,
    disp_s,
    x_v,
    z_v,
    keep_v,
    rs_s,
    rs_r,
    rs_as,
    rs_ar,
    ret_s,
    ret_r,
    w_sem,
    pack_ss,
    pack_rs,
    att_ss,
    att_rs,
    mix_ss,
    mix_rs,
    disp_ss,
    x_rs,
    fwd_ss,
    rs_ss,
    rs_rs,
    ret_ss,
    ret_rs,
):
    n_sp, n_tp, tok, hd, cap, own = dims
    me = lax.axis_index("sp")
    t = lax.axis_index("tp")
    sib = t + 1 - 2 * (t % 2)
    acr = (t + 2) % n_tp
    far = (sib + 2) % n_tp
    width = n_tp * own

    def send(src, dst, ss, rs, sp_id, tp_id):
        return pltpu.make_async_remote_copy(
            src_ref=src,
            dst_ref=dst,
            send_sem=ss,
            recv_sem=rs,
            device_id=(sp_id, tp_id),
            device_id_type=MESH,
        )

    def cols(index):
        return pl.ds(pl.multiple_of(index * own, own), own)

    loads = [
        pltpu.make_async_copy(ow_hbm, ow_v, w_sem.at[0]),
        pltpu.make_async_copy(res_hbm.at[:, cols(t)], res_v, w_sem.at[1]),
        pltpu.make_async_copy(gw_hbm.at[0], gw_v, w_sem.at[2]),
        pltpu.make_async_copy(uw_hbm.at[0], uw_v, w_sem.at[3]),
        pltpu.make_async_copy(dw_hbm.at[0], dw_v, w_sem.at[4]),
    ]
    for load in loads:
        load.start()

    barrier = pltpu.get_barrier_semaphore()
    for d in range(1, n_sp):
        pl.semaphore_signal(
            barrier, inc=1, device_id=((me + d) % n_sp, t), device_id_type=MESH
        )
    for peer in (sib, acr):
        pl.semaphore_signal(barrier, inc=1, device_id=(me, peer), device_id_type=MESH)

    half = tok // 2
    for h in range(n_sp):
        lanes = slice(h * hd, (h + 1) * hd)
        q_h = q_ref[:, lanes].astype(f32)
        k_h = k_ref[:, lanes].astype(f32)
        v_h = v_ref[:, lanes].astype(f32)
        pack_s[h, 0:tok, :] = jnp.concatenate([q_h, k_h], axis=1).astype(bf16)
        pack_s[h, tok : tok + half, :] = jnp.concatenate([v_h[:half], v_h[half:]], axis=1).astype(
            bf16
        )
        pack_s[h, tok + half : tok + half + 16, :] = jnp.broadcast_to(
            bias_ref[h : h + 1, :].astype(f32), (16, tok)
        ).astype(bf16)
    pl.semaphore_wait(barrier, n_sp + 1)

    def pack_copy(block, peer, slot):
        return send(
            pack_s.at[block], pack_r.at[slot], pack_ss.at[block], pack_rs.at[slot], peer, t
        )

    for d in range(1, n_sp):
        peer = (me + d) % n_sp
        pack_copy(peer, peer, me).start()
    pack_r[me] = pack_s[me]

    ids0 = ids_ref[:, 0:1]
    ids1 = ids_ref[:, 1:2]
    lane = lax.broadcasted_iota(jnp.int32, (tok, 128), 1)
    row = lax.broadcasted_iota(jnp.int32, (tok, tok), 0)
    col = lax.broadcasted_iota(jnp.int32, (tok, tok), 1)
    named0 = (lane == ids0).astype(f32)
    named1 = (lane == ids1).astype(f32)
    earlier = (col < row).astype(f32).astype(bf16)
    count = jnp.dot(earlier, (named0 + named1).astype(bf16), preferred_element_type=f32)
    slot0 = jnp.sum(named0 * count, axis=1, keepdims=True) + (ids0 * cap).astype(f32)
    slot1 = jnp.sum(named1 * count, axis=1, keepdims=True) + (ids1 * cap).astype(f32)
    slots = lax.broadcasted_iota(jnp.int32, (tok, n_sp * cap), 1).astype(f32)
    pick0 = (slots == slot0).astype(f32)
    pick1 = (slots == slot1).astype(f32)

    qb = 2 * tok
    row = lax.broadcasted_iota(jnp.int32, (qb, qb), 0)
    col = lax.broadcasted_iota(jnp.int32, (qb, qb), 1)
    causal = col < row
    tri = (row >= col).astype(f32).astype(bf16)
    bias_rows = []
    for i in range(n_sp // 2):
        blocks = []
        v_blocks = []
        bias_i = []
        for b in (2 * i, 2 * i + 1):

            @pl.when(b != me)
            def _():
                pack_copy(b, b, b).wait_recv()

            blocks.append(pack_r[b, 0:tok, :].astype(f32))
            vp = pack_r[b, tok : tok + half, :].astype(f32)
            v_blocks += [vp[:, :hd], vp[:, hd:]]
            bias_i.append(pack_r[b, tok + half : tok + half + 16, :].astype(f32)[0:1])
        both = jnp.concatenate(blocks, axis=0)
        q_i = both[:, :hd]
        k_i = both[:, hd:]
        q_i = q_i * lax.rsqrt(jnp.mean(q_i * q_i, axis=1, keepdims=True) + epsilon) * qg_ref[...]
        k_i = k_i * lax.rsqrt(jnp.mean(k_i * k_i, axis=1, keepdims=True) + epsilon) * kg_ref[...]
        q_n = (q_i.astype(bf16).astype(f32) * hd**-0.5).astype(bf16)
        kn_v[i] = k_i.astype(bf16)
        vn_v[i] = jnp.concatenate(v_blocks, axis=0).astype(bf16)
        bias_rows.append(jnp.concatenate(bias_i, axis=1))
        summed = jnp.zeros((qb, hd), f32)
        carry = jnp.zeros((qb, 1), f32)
        for j in range(i, -1, -1):
            s = lax.dot_general(
                q_n, kn_v[j], (((1,), (1,)), ((), ())), preferred_element_type=f32
            )
            s = s - bias_rows[j]
            leave = jnp.maximum(s, 0.0) + jnp.log(1.0 + jnp.exp(-jnp.abs(s)))
            if j == i:
                leave = jnp.where(causal, leave, 0.0)
            top = leave.astype(bf16)
            low = (leave - top.astype(f32)).astype(bf16)
            total = jnp.dot(top, tri, preferred_element_type=f32) + jnp.dot(
                low, tri, preferred_element_type=f32
            )
            weight = jnp.exp(s - total - carry)
            if j == i:
                weight = jnp.where(causal, weight, 0.0)
            carry = carry + total[:, 0:1]
            summed = summed + jnp.dot(weight.astype(bf16), vn_v[j], preferred_element_type=f32)
        for b in (2 * i, 2 * i + 1):
            part = summed[(b - 2 * i) * tok : (b - 2 * i + 1) * tok]
            packed = jnp.concatenate([part[:half], part[half:]], axis=1).astype(bf16)
            att_s[b] = packed

            @pl.when(b != me)
            def _():
                send(att_s.at[b], att_r.at[me], att_ss.at[b], att_rs.at[me], b, t).start()

            @pl.when(b == me)
            def _():
                att_r[b] = packed

    for h in range(n_sp):

        @pl.when(h != me)
        def _():
            send(att_s.at[h], att_r.at[h], att_ss.at[h], att_rs.at[h], h, t).wait_recv()

    heads = []
    for h in range(n_sp):
        p = att_r[h].astype(f32)
        heads.append(jnp.concatenate([p[:, :hd], p[:, hd:]], axis=0))
    attended = jnp.concatenate(heads, axis=1).astype(bf16)

    loads[0].wait()

    def project(index):
        return jnp.dot(attended, ow_v[:, cols(index)], preferred_element_type=f32)

    def mix_copy(slot):
        return send(mix_s.at[slot], mix_r.at[slot], mix_ss.at[slot], mix_rs.at[slot], me, sib)

    mix_s[1] = project(far).astype(bf16)
    mix_copy(1).start()
    mix_s[0] = project(sib).astype(bf16)
    mix_copy(0).start()
    across = project(acr)
    mix_copy(1).wait_recv()
    mix_as[...] = (across + mix_r[1].astype(f32)).astype(bf16)
    mix_over = send(mix_as, mix_ar, mix_ss.at[2], mix_rs.at[2], me, acr)
    mix_over.start()
    mixed = project(t)
    loads[1].wait()
    mix_copy(0).wait_recv()
    mixed = mixed + mix_r[0].astype(f32) + res_v[...].astype(f32)
    mix_over.wait_recv()
    own_b = (mixed + mix_ar[...].astype(f32)).astype(bf16)

    spread = lax.dot_general(
        (pick0 + pick1).astype(bf16), own_b, (((0,), (0,)), ((), ())), preferred_element_type=f32
    )
    for e in range(n_sp):
        disp_s[e] = spread[e * cap : (e + 1) * cap].astype(bf16)

    quad = n_sp // 2
    base_near = (me // quad) * quad
    base_away = (base_near + quad) % n_sp

    def disp_copy(block, peer, slot):
        return send(
            disp_s.at[block], x_v.at[t, slot], disp_ss.at[block], x_rs.at[t, slot], peer, t
        )

    away = [base_away + (me + g) % quad for g in range(quad)]
    near = [base_near + (me + g) % quad for g in range(quad)]
    order = []
    for g in range(1, quad):
        order += [near[g], away[g]]
    for peer in order + [away[0]]:
        disp_copy(peer, peer, me).start()
    x_v[t, me] = disp_s[me]

    def pass_sib(column, src, sem):
        return send(
            x_v.at[column, src],
            x_v.at[column, src],
            fwd_ss.at[sem, src],
            x_rs.at[column, src],
            me,
            sib,
        )

    def pass_acr(src):
        return send(x_v.at[t, src], x_v.at[t, src], fwd_ss.at[1, src], x_rs.at[t, src], me, acr)

    def came(column, src):
        send(
            x_v.at[column, src], x_v.at[column, src], fwd_ss.at[0, src], x_rs.at[column, src], me, sib
        ).wait_recv()

    def first_pass(srcs, skip_first):
        for g, src in enumerate(srcs):
            if not (skip_first and g == 0):
                came(t, src)
            pass_acr(src).start()
            pass_sib(t, src, 0).start()

    def second_pass(srcs):
        for src in srcs:
            came(acr, src)
            pass_sib(acr, src, 2).start()

    def expert_share(group, srcs):
        for src in srcs:
            came(sib, src)
            came(far, src)
        base = base_near if group == 0 else base_away
        pieces = []
        for g in range(quad):
            pieces.append(
                jnp.concatenate([x_v[c, base + g].astype(f32) for c in range(n_tp)], axis=1)
            )
        rows = jnp.concatenate(pieces, axis=0)
        scale = lax.rsqrt(jnp.mean(rows * rows, axis=1, keepdims=True) + epsilon)
        z_v[...] = (rows * scale * ng_ref[...]).astype(bf16)
        if group == 0:
            loads[2].wait()
            loads[3].wait()
        gate_pre = jnp.dot(z_v[...], gw_v[...], preferred_element_type=f32)
        up_pre = jnp.dot(z_v[...], uw_v[...], preferred_element_type=f32)
        hidden = activate(gate_pre, up_pre).astype(bf16)
        if group == 0:
            loads[4].wait()

        def down(index):
            return jnp.dot(hidden, dw_v[:, cols(index)], preferred_element_type=f32)

        rs_s[group, 1] = down(far).astype(bf16)
        rs_copy(group, 1).start()
        rs_s[group, 0] = down(sib).astype(bf16)
        rs_copy(group, 0).start()
        keep_v[group, 1] = down(acr)
        keep_v[group, 0] = down(t)

    def rs_copy(group, slot):
        return send(
            rs_s.at[group, slot],
            rs_r.at[group, slot],
            rs_ss.at[group, slot],
            rs_rs.at[group, slot],
            me,
            sib,
        )

    def rs_over(group):
        return send(
            rs_as.at[group], rs_ar.at[group], rs_ss.at[group, 2], rs_rs.at[group, 2], me, acr
        )

    def step_over(group):
        rs_copy(group, 1).wait_recv()
        rs_as[group] = (keep_v[group, 1] + rs_r[group, 1].astype(f32)).astype(bf16)
        rs_over(group).start()

    def ret_copy(block, peer, slot):
        return send(ret_s.at[block], ret_r.at[slot], ret_ss.at[block], ret_rs.at[slot], peer, t)

    def step_back(group):
        rs_copy(group, 0).wait_recv()
        part = keep_v[group, 0] + rs_r[group, 0].astype(f32)
        rs_over(group).wait_recv()
        part = part + rs_ar[group].astype(f32)
        base = base_near if group == 0 else base_away
        for g in range(quad):
            src = base + g
            rows = part[g * cap : (g + 1) * cap].astype(bf16)
            ret_s[src] = rows
            if group == 0:

                @pl.when(src != me)
                def _():
                    ret_copy(src, src, me).start()

                @pl.when(src == me)
                def _():
                    ret_r[src] = rows

            else:
                ret_copy(src, src, me).start()

    first_pass(near, True)
    second_pass(near)
    first_pass(away, False)
    expert_share(0, near)
    second_pass(away)
    step_over(0)
    expert_share(1, away)
    step_back(0)
    step_over(1)
    step_back(1)

    for d in range(1, n_sp):
        src = (me + d) % n_sp
        ret_copy(src, src, src).wait_recv()
    back = jnp.concatenate([ret_r[e].astype(f32) for e in range(n_sp)], axis=0).astype(bf16)
    taken0 = jnp.dot(pick0.astype(bf16), back, preferred_element_type=f32)
    taken1 = jnp.dot(pick1.astype(bf16), back, preferred_element_type=f32)
    routed = taken0 * rw_ref[:, 0:1] + taken1 * rw_ref[:, 1:2]
    out_ref[...] = (own_b.astype(f32) + routed).astype(bf16)

    for d in range(1, n_sp):
        peer = (me + d) % n_sp
        pack_copy(peer, peer, me).wait_send()
        send(att_s.at[peer], att_r.at[me], att_ss.at[peer], att_rs.at[me], peer, t).wait_send()
        disp_copy(peer, peer, me).wait_send()
        ret_copy(peer, peer, me).wait_send()
    mix_copy(0).wait_send()
    mix_copy(1).wait_send()
    mix_over.wait_send()
    for src in range(n_sp):
        pass_acr(src).wait_send()
        pass_sib(t, src, 0).wait_send()
        pass_sib(acr, src, 2).wait_send()
    for group in range(2):
        rs_copy(group, 0).wait_send()
        rs_copy(group, 1).wait_send()
        rs_over(group).wait_send()


def fused_device(n_sp, n_tp, *args):
    (
        residual,
        queries,
        keys,
        values,
        stick_bias,
        query_gain,
        key_gain,
        out_weight,
        norm_gain,
        route_ids,
        route_weights,
        gate_weight,
        up_weight,
        down_weight,
    ) = args
    tok, packed = queries.shape
    hd = query_gain.shape[0]
    model = residual.shape[1]
    own = model // n_tp
    hidden = gate_weight.shape[2]
    picks = route_ids.shape[1]
    cap = (5 * tok * picks + 4 * n_sp - 1) // (4 * n_sp)
    quad = n_sp // 2
    pairs = n_sp // 2
    half = tok // 2
    vmem = pl.BlockSpec(memory_space=pltpu.VMEM)
    anywhere = pl.BlockSpec(memory_space=pl.ANY)
    dma = pltpu.SemaphoreType.DMA
    scratch = [
        pltpu.VMEM((tok, own), bf16),
        pltpu.VMEM((packed, model), bf16),
        pltpu.VMEM((model, hidden), bf16),
        pltpu.VMEM((model, hidden), bf16),
        pltpu.VMEM((hidden, model), bf16),
        pltpu.VMEM((n_sp, tok + half + 16, 2 * hd), bf16),
        pltpu.VMEM((n_sp, tok + half + 16, 2 * hd), bf16),
        pltpu.VMEM((pairs, 2 * tok, hd), bf16),
        pltpu.VMEM((pairs, 2 * tok, hd), bf16),
        pltpu.VMEM((n_sp, half, 2 * hd), bf16),
        pltpu.VMEM((n_sp, half, 2 * hd), bf16),
        pltpu.VMEM((2, tok, own), bf16),
        pltpu.VMEM((2, tok, own), bf16),
        pltpu.VMEM((tok, own), bf16),
        pltpu.VMEM((tok, own), bf16),
        pltpu.VMEM((n_sp, cap, own), bf16),
        pltpu.VMEM((n_tp, n_sp, cap, own), bf16),
        pltpu.VMEM((quad * cap, model), bf16),
        pltpu.VMEM((2, 2, quad * cap, own), f32),
        pltpu.VMEM((2, 2, quad * cap, own), bf16),
        pltpu.VMEM((2, 2, quad * cap, own), bf16),
        pltpu.VMEM((2, quad * cap, own), bf16),
        pltpu.VMEM((2, quad * cap, own), bf16),
        pltpu.VMEM((n_sp, cap, own), bf16),
        pltpu.VMEM((n_sp, cap, own), bf16),
        dma((5,)),
        dma((n_sp,)),
        dma((n_sp,)),
        dma((n_sp,)),
        dma((n_sp,)),
        dma((3,)),
        dma((3,)),
        dma((n_sp,)),
        dma((n_tp, n_sp)),
        dma((3, n_sp)),
        dma((2, 3)),
        dma((2, 3)),
        dma((n_sp,)),
        dma((n_sp,)),
    ]
    return pl.pallas_call(
        functools.partial(fused_kernel, (n_sp, n_tp, tok, hd, cap, own)),
        out_shape=jax.ShapeDtypeStruct((tok, own), bf16),
        in_specs=[vmem] * 9 + [anywhere] * 5,
        out_specs=vmem,
        scratch_shapes=scratch,
        compiler_params=pltpu.CompilerParams(
            collective_id=0, has_side_effects=True, vmem_limit_bytes=56 * 1024 * 1024
        ),
    )(
        queries,
        keys,
        values,
        stick_bias,
        query_gain.reshape(1, -1),
        key_gain.reshape(1, -1),
        norm_gain.reshape(1, -1),
        route_ids,
        route_weights,
        residual,
        out_weight,
        gate_weight,
        up_weight,
        down_weight,
    )


def device_program(n_sp, n_tp, *args):
    tok, packed = args[1].shape
    hd = args[5].shape[0]
    picks = args[9].shape[1]
    cap = (5 * tok * picks + 4 * n_sp - 1) // (4 * n_sp)
    fits = (
        packed == n_sp * hd
        and tok == 2 * hd == 128
        and cap % 8 == 0
        and n_tp == 4
        and n_sp % 4 == 0
        and picks == 2
        and args[11].shape[0] == 1
    )
    if fits:
        return fused_device(n_sp, n_tp, *args)
    return per_device(*args)


def solution(mesh):
    placed = (
        P("sp", None),
        P("sp", "tp"),
        P("sp", "tp"),
        P("sp", "tp"),
        P("tp", "sp"),
        P(),
        P(),
        P("tp", None),
        P(),
        P("sp", None),
        P("sp", None),
        P("sp", None, "tp"),
        P("sp", None, "tp"),
        P("sp", "tp", None),
    )
    return jax.shard_map(
        functools.partial(device_program, mesh.shape["sp"], mesh.shape["tp"]),
        mesh=mesh, in_specs=placed, out_specs=P("sp", "tp"), check_vma=False
    )
```

```python
import functools
import math

import jax
import jax.numpy as jnp
from jax import lax
from jax.experimental import pallas as pl
from jax.experimental.pallas import tpu as pltpu
from jax.sharding import PartitionSpec as P

epsilon = 1e-06
clamp_limit = 7.0
swish_scale = 1.702


def head_normalize(packed, gain):
    values_f = packed.astype(jnp.float32).reshape(packed.shape[0], -1, gain.shape[0])
    scaled = (
        values_f * lax.rsqrt(jnp.mean(values_f * values_f, axis=-1, keepdims=True) + epsilon) * gain
    )
    return scaled.astype(jnp.bfloat16)


def activate(gate_pre, up_pre):
    gate_top = jnp.minimum(gate_pre, clamp_limit)
    up_clip = jnp.clip(up_pre, -clamp_limit, clamp_limit)
    return (up_clip + 1.0) * (gate_top * jax.nn.sigmoid(swish_scale * gate_top))


def slot_table(picked, expert_count, capacity):
    flat_ids = picked.reshape(-1)
    one_hot = (flat_ids[:, None] == jnp.arange(expert_count, dtype=jnp.int32)[None, :]).astype(
        jnp.int32
    )
    before = jnp.sum((jnp.cumsum(one_hot, axis=0) - one_hot) * one_hot, axis=1)
    return flat_ids * capacity + before


def key_block(state_pair, queries_n, keys_block, values_block, bias_block, first_key, query_pos):
    summed, log_carry = state_pair
    key_count = bias_block.shape[1]
    head_total = bias_block.shape[0]
    keys_heads = keys_block.reshape(key_count, head_total, -1)
    values_heads = values_block.reshape(key_count, head_total, -1)
    head_dim = keys_heads.shape[2]
    scores = jnp.einsum(
        "qhd,khd->hqk", queries_n, keys_heads, preferred_element_type=jnp.float32
    ) * head_dim ** (-0.5)
    scores = scores - bias_block.astype(jnp.float32)[:, None, :]
    key_pos = first_key + jnp.arange(key_count, dtype=jnp.int32)
    causal = ((key_pos[None, :] < query_pos[:, None]) & (key_pos[None, :] >= 0))[None]
    log_stay = jnp.where(causal, jax.nn.log_sigmoid(-scores), 0.0)
    later_sum = lax.cumsum(log_stay, axis=2, reverse=True) - log_stay
    weight = jnp.where(
        causal, jnp.exp(jax.nn.log_sigmoid(scores) + later_sum + log_carry[:, :, None]), 0.0
    )
    summed = summed + jnp.einsum(
        "hqk,khd->qhd",
        weight.astype(jnp.bfloat16),
        values_heads,
        preferred_element_type=jnp.float32,
    )
    return (summed, log_carry + jnp.sum(log_stay, axis=2))


def per_device(
    residual,
    queries,
    keys,
    values,
    stick_bias,
    query_gain,
    key_gain,
    out_weight,
    norm_gain,
    route_ids,
    route_weights,
    gate_weight,
    up_weight,
    down_weight,
):
    tok_rows = queries.shape[0]
    width_sp = lax.axis_size("sp")
    offset = lax.axis_index("sp") * tok_rows
    query_pos = offset + jnp.arange(tok_rows, dtype=jnp.int32)
    queries_n = head_normalize(queries, query_gain)
    keys_n = head_normalize(keys, key_gain).reshape(tok_rows, -1)
    head_total = stick_bias.shape[0]
    head_dim = query_gain.shape[0]
    state_pair = (
        jnp.zeros((tok_rows, head_total, head_dim), jnp.float32),
        jnp.zeros((head_total, tok_rows), jnp.float32),
    )
    all_keys, all_values, all_bias = (
        lax.all_gather(keys_n, "sp", axis=0, tiled=True),
        lax.all_gather(values, "sp", axis=0, tiled=True),
        lax.all_gather(stick_bias, "sp", axis=1, tiled=True),
    )
    key_total = all_keys.shape[0]
    block_len = math.gcd(key_total, 512)
    block_total = key_total // block_len

    def sweep_block(block_step, running):
        first_key = (block_total - 1 - block_step) * block_len
        return key_block(
            running,
            queries_n,
            lax.dynamic_slice_in_dim(all_keys, first_key, block_len, 0),
            lax.dynamic_slice_in_dim(all_values, first_key, block_len, 0),
            lax.dynamic_slice_in_dim(all_bias, first_key, block_len, 1),
            first_key,
            query_pos,
        )

    state_pair = lax.fori_loop(0, block_total, sweep_block, state_pair)
    attended = state_pair[0].reshape(tok_rows, head_total * head_dim).astype(jnp.bfloat16)
    partial_value = jnp.dot(attended, out_weight, preferred_element_type=jnp.float32)
    model_width = residual.shape[1]
    expert_count = width_sp * gate_weight.shape[0]
    pick_count = route_ids.shape[1]
    capacity = (5 * tok_rows * pick_count + 4 * expert_count - 1) // (4 * expert_count)
    slot_index = slot_table(route_ids, expert_count, capacity)
    assigned = slot_index.shape[0]
    source = (
        jnp.zeros((expert_count * capacity,), jnp.int32)
        .at[slot_index]
        .set(jnp.arange(assigned, dtype=jnp.int32) // pick_count)
    )
    filled = (
        jnp.zeros((expert_count * capacity,), jnp.bfloat16)
        .at[slot_index]
        .set(jnp.ones((assigned,), jnp.bfloat16))
    )
    gate_local = gate_weight[0]
    up_local = up_weight[0]
    down_local = down_weight[0]
    mixed_share = lax.psum_scatter(
        partial_value.astype(jnp.bfloat16), "tp", scatter_dimension=1, tiled=True
    ).astype(jnp.float32)
    own_width = mixed_share.shape[1]
    col_start = lax.axis_index("tp") * own_width
    own_res = lax.dynamic_slice_in_dim(residual, col_start, own_width, 1).astype(jnp.float32)
    own_cols = (own_res + mixed_share).astype(jnp.bfloat16).astype(jnp.float32)
    square_total = lax.psum(jnp.sum(own_cols * own_cols, axis=1), "tp")
    gain_cols = lax.dynamic_slice_in_dim(norm_gain, col_start, own_width, 0)
    normed_share = (
        own_cols * lax.rsqrt(square_total / model_width + epsilon)[:, None] * gain_cols
    ).astype(jnp.bfloat16)
    outgoing = (normed_share[source] * filled[:, None]).reshape(expert_count, capacity, -1)
    piece = lax.all_gather(
        lax.all_to_all(outgoing, "sp", split_axis=0, concat_axis=0, tiled=True),
        "tp",
        axis=2,
        tiled=True,
    )
    gate_pre = jnp.einsum("scd,df->scf", piece, gate_local, preferred_element_type=jnp.float32)
    up_pre = jnp.einsum("scd,df->scf", piece, up_local, preferred_element_type=jnp.float32)
    hidden = activate(gate_pre, up_pre).astype(jnp.bfloat16)
    share = jnp.einsum("scf,fd->scd", hidden, down_local, preferred_element_type=jnp.float32)
    returned = lax.psum_scatter(share.astype(jnp.bfloat16), "tp", scatter_dimension=2, tiled=True)
    arrived = lax.all_to_all(returned, "sp", split_axis=0, concat_axis=0, tiled=True)
    columns = arrived.shape[2]
    taken_rows = arrived.reshape(expert_count * capacity, columns)[slot_index]
    taken_rows = taken_rows.astype(jnp.float32).reshape(tok_rows, pick_count, columns)
    routed = jnp.sum(taken_rows * route_weights[:, :, None], axis=1)
    return (own_cols + routed).astype(jnp.bfloat16)


f32 = jnp.float32
bf16 = jnp.bfloat16
MESH = pl.DeviceIdType.MESH


def fused_kernel(
    dims,
    q_ref,
    k_ref,
    v_ref,
    bias_ref,
    qg_ref,
    kg_ref,
    ng_ref,
    ids_ref,
    rw_ref,
    res_hbm,
    ow_hbm,
    gw_hbm,
    uw_hbm,
    dw_hbm,
    out_ref,
    res_v,
    ow_v,
    gw_v,
    uw_v,
    dw_v,
    pack_s,
    pack_r,
    kn_v,
    vn_v,
    att_s,
    att_r,
    mix_s,
    mix_r,
    mix_as,
    mix_ar,
    disp_s,
    x_v,
    z_v,
    keep_v,
    rs_s,
    rs_r,
    rs_as,
    rs_ar,
    ret_s,
    ret_r,
    w_sem,
    pack_ss,
    pack_rs,
    att_ss,
    att_rs,
    mix_ss,
    mix_rs,
    disp_ss,
    x_rs,
    fwd_ss,
    rs_ss,
    rs_rs,
    over_ss,
    over_rs,
    ret_ss,
    ret_rs,
):
    n_sp, n_tp, tok, hd, cap, own = dims
    me = lax.axis_index("sp")
    t = lax.axis_index("tp")
    sib = t + 1 - 2 * (t % 2)
    acr = (t + 2) % n_tp
    far = (sib + 2) % n_tp
    width = n_tp * own

    def send(src, dst, ss, rs, sp_id, tp_id):
        return pltpu.make_async_remote_copy(
            src_ref=src,
            dst_ref=dst,
            send_sem=ss,
            recv_sem=rs,
            device_id=(sp_id, tp_id),
            device_id_type=MESH,
        )

    def cols(index):
        return pl.ds(pl.multiple_of(index * own, own), own)

    loads = [
        pltpu.make_async_copy(ow_hbm, ow_v, w_sem.at[0]),
        pltpu.make_async_copy(res_hbm.at[:, cols(t)], res_v, w_sem.at[1]),
        pltpu.make_async_copy(gw_hbm.at[0], gw_v, w_sem.at[2]),
        pltpu.make_async_copy(uw_hbm.at[0], uw_v, w_sem.at[3]),
        pltpu.make_async_copy(dw_hbm.at[0], dw_v, w_sem.at[4]),
    ]
    for load in loads:
        load.start()

    barrier = pltpu.get_barrier_semaphore()
    for d in range(1, n_sp):
        pl.semaphore_signal(
            barrier, inc=1, device_id=((me + d) % n_sp, t), device_id_type=MESH
        )
    for peer in (sib, acr):
        pl.semaphore_signal(barrier, inc=1, device_id=(me, peer), device_id_type=MESH)

    half = tok // 2
    for h in range(n_sp):
        lanes = slice(h * hd, (h + 1) * hd)
        q_h = q_ref[:, lanes].astype(f32)
        k_h = k_ref[:, lanes].astype(f32)
        v_h = v_ref[:, lanes].astype(f32)
        pack_s[h, 0:tok, :] = jnp.concatenate([q_h, k_h], axis=1).astype(bf16)
        pack_s[h, tok : tok + half, :] = jnp.concatenate([v_h[:half], v_h[half:]], axis=1).astype(
            bf16
        )
        pack_s[h, tok + half : tok + half + 16, :] = jnp.broadcast_to(
            bias_ref[h : h + 1, :].astype(f32), (16, tok)
        ).astype(bf16)
    pl.semaphore_wait(barrier, n_sp + 1)

    def pack_copy(block, peer, slot):
        return send(
            pack_s.at[block], pack_r.at[slot], pack_ss.at[block], pack_rs.at[slot], peer, t
        )

    for d in range(1, n_sp):
        peer = (me + d) % n_sp
        pack_copy(peer, peer, me).start()
    pack_r[me] = pack_s[me]

    by_token = jnp.transpose(
        jnp.concatenate(
            [ids_ref[...].astype(f32), rw_ref[...], jnp.zeros((4, tok), f32)], axis=0
        )
    )
    ids0 = by_token[:, 0:1]
    ids1 = by_token[:, 1:2]
    lane = lax.broadcasted_iota(jnp.int32, (tok, 128), 1).astype(f32)
    row = lax.broadcasted_iota(jnp.int32, (tok, tok), 0)
    col = lax.broadcasted_iota(jnp.int32, (tok, tok), 1)
    named0 = (lane == ids0).astype(f32)
    named1 = (lane == ids1).astype(f32)
    earlier = (col < row).astype(f32).astype(bf16)
    count = jnp.dot(earlier, (named0 + named1).astype(bf16), preferred_element_type=f32)
    slot0 = jnp.sum(named0 * count, axis=1, keepdims=True) + ids0 * cap
    slot1 = jnp.sum(named1 * count, axis=1, keepdims=True) + ids1 * cap
    slots = lax.broadcasted_iota(jnp.int32, (tok, n_sp * cap), 1).astype(f32)
    pick0 = (slots == slot0).astype(f32)
    pick1 = (slots == slot1).astype(f32)

    qb = 2 * tok
    row = lax.broadcasted_iota(jnp.int32, (qb, qb), 0)
    col = lax.broadcasted_iota(jnp.int32, (qb, qb), 1)
    causal = col < row
    tri = (row >= col).astype(f32).astype(bf16)
    bias_rows = []
    for i in range(n_sp // 2):
        blocks = []
        v_blocks = []
        bias_i = []
        for b in (2 * i, 2 * i + 1):

            @pl.when(b != me)
            def _():
                pack_copy(b, b, b).wait_recv()

            blocks.append(pack_r[b, 0:tok, :].astype(f32))
            vp = pack_r[b, tok : tok + half, :].astype(f32)
            v_blocks += [vp[:, :hd], vp[:, hd:]]
            bias_i.append(pack_r[b, tok + half : tok + half + 16, :].astype(f32)[0:1])
        both = jnp.concatenate(blocks, axis=0)
        q_i = both[:, :hd]
        k_i = both[:, hd:]
        q_i = q_i * lax.rsqrt(jnp.mean(q_i * q_i, axis=1, keepdims=True) + epsilon) * qg_ref[...]
        k_i = k_i * lax.rsqrt(jnp.mean(k_i * k_i, axis=1, keepdims=True) + epsilon) * kg_ref[...]
        q_n = (q_i.astype(bf16).astype(f32) * hd**-0.5).astype(bf16)
        kn_v[i] = k_i.astype(bf16)
        vn_v[i] = jnp.concatenate(v_blocks, axis=0).astype(bf16)
        bias_rows.append(jnp.concatenate(bias_i, axis=1))
        summed = jnp.zeros((qb, hd), f32)
        carry = jnp.zeros((qb, 1), f32)
        for j in range(i, -1, -1):
            s = lax.dot_general(
                q_n, kn_v[j], (((1,), (1,)), ((), ())), preferred_element_type=f32
            )
            s = s - bias_rows[j]
            leave = jnp.maximum(s, 0.0) + jnp.log(1.0 + jnp.exp(-jnp.abs(s)))
            if j == i:
                leave = jnp.where(causal, leave, 0.0)
            top = leave.astype(bf16)
            low = (leave - top.astype(f32)).astype(bf16)
            total = jnp.dot(top, tri, preferred_element_type=f32) + jnp.dot(
                low, tri, preferred_element_type=f32
            )
            weight = jnp.exp(s - total - carry)
            if j == i:
                weight = jnp.where(causal, weight, 0.0)
            carry = carry + total[:, 0:1]
            summed = summed + jnp.dot(weight.astype(bf16), vn_v[j], preferred_element_type=f32)
        for b in (2 * i, 2 * i + 1):
            part = summed[(b - 2 * i) * tok : (b - 2 * i + 1) * tok]
            packed = jnp.concatenate([part[:half], part[half:]], axis=1).astype(bf16)
            att_s[b] = packed

            @pl.when(b != me)
            def _():
                send(att_s.at[b], att_r.at[me], att_ss.at[b], att_rs.at[me], b, t).start()

            @pl.when(b == me)
            def _():
                att_r[b] = packed

    for h in range(n_sp):

        @pl.when(h != me)
        def _():
            send(att_s.at[h], att_r.at[h], att_ss.at[h], att_rs.at[h], h, t).wait_recv()

    heads = []
    for h in range(n_sp):
        p = att_r[h].astype(f32)
        heads.append(jnp.concatenate([p[:, :hd], p[:, hd:]], axis=0))
    attended = jnp.concatenate(heads, axis=1).astype(bf16)

    loads[0].wait()

    def project(index):
        return jnp.dot(attended, ow_v[:, cols(index)], preferred_element_type=f32)

    def mix_copy(slot):
        return send(mix_s.at[slot], mix_r.at[slot], mix_ss.at[slot], mix_rs.at[slot], me, sib)

    mix_s[1] = project(far).astype(bf16)
    mix_copy(1).start()
    mix_s[0] = project(sib).astype(bf16)
    mix_copy(0).start()
    across = project(acr)
    mix_copy(1).wait_recv()
    mix_as[...] = (across + mix_r[1].astype(f32)).astype(bf16)
    mix_over = send(mix_as, mix_ar, mix_ss.at[2], mix_rs.at[2], me, acr)
    mix_over.start()
    mixed = project(t)
    loads[1].wait()
    mix_copy(0).wait_recv()
    mixed = mixed + mix_r[0].astype(f32) + res_v[...].astype(f32)
    mix_over.wait_recv()
    own_b = (mixed + mix_ar[...].astype(f32)).astype(bf16)

    spread = lax.dot_general(
        (pick0 + pick1).astype(bf16), own_b, (((0,), (0,)), ((), ())), preferred_element_type=f32
    )
    for e in range(n_sp):
        disp_s[e] = spread[e * cap : (e + 1) * cap].astype(bf16)

    quad = n_sp // 2
    line = me // 2
    side = me % 2
    lines = [line, line + 1 - 2 * (line % 2), (line + 2) % quad, quad - 1 - line]
    groups = [[2 * at + side for at in lines], [2 * at + 1 - side for at in lines]]

    def disp_copy(block, peer, slot):
        return send(
            disp_s.at[block], x_v.at[t, slot], disp_ss.at[block], x_rs.at[t, slot], peer, t
        )

    for peer in groups[0][1:] + groups[1]:
        disp_copy(peer, peer, me).start()
    x_v[t, me] = disp_s[me]

    def pass_sib(column, src, sem):
        return send(
            x_v.at[column, src],
            x_v.at[column, src],
            fwd_ss.at[sem, src],
            x_rs.at[column, src],
            me,
            sib,
        )

    def pass_acr(src):
        return send(x_v.at[t, src], x_v.at[t, src], fwd_ss.at[1, src], x_rs.at[t, src], me, acr)

    def came(column, src):
        send(
            x_v.at[column, src], x_v.at[column, src], fwd_ss.at[0, src], x_rs.at[column, src], me, sib
        ).wait_recv()

    def first_pass(srcs, skip_first):
        for g, src in enumerate(srcs):
            if not (skip_first and g == 0):
                came(t, src)
            pass_acr(src).start()
            pass_sib(t, src, 0).start()

    def second_pass(srcs):
        for src in srcs:
            came(acr, src)
            pass_sib(acr, src, 2).start()

    def expert_share(group, srcs):
        for src in srcs:
            came(sib, src)
            came(far, src)
        pieces = []
        for src in srcs:
            pieces.append(jnp.concatenate([x_v[c, src].astype(f32) for c in range(n_tp)], axis=1))
        rows = jnp.concatenate(pieces, axis=0)
        scale = lax.rsqrt(jnp.mean(rows * rows, axis=1, keepdims=True) + epsilon)
        z_v[...] = (rows * scale * ng_ref[...]).astype(bf16)
        if group == 0:
            loads[2].wait()
            loads[3].wait()
        gate_pre = jnp.dot(z_v[...], gw_v[...], preferred_element_type=f32)
        up_pre = jnp.dot(z_v[...], uw_v[...], preferred_element_type=f32)
        hidden = activate(gate_pre, up_pre).astype(bf16)
        if group == 0:
            loads[4].wait()

        def down(index):
            return jnp.dot(hidden, dw_v[:, cols(index)], preferred_element_type=f32)

        rs_s[group, 1] = down(far).astype(bf16)
        rs_copy(group, 1).start()
        rs_s[group, 0] = down(sib).astype(bf16)
        rs_copy(group, 0).start()
        keep_v[group, 1] = down(acr)
        keep_v[group, 0] = down(t)

    def rs_copy(group, slot):
        return send(
            rs_s.at[group, slot],
            rs_r.at[group, slot],
            rs_ss.at[group, slot],
            rs_rs.at[group, slot],
            me,
            sib,
        )

    def rs_over(group, g):
        return send(
            rs_as.at[group, g], rs_ar.at[group, g], over_ss.at[group, g], over_rs.at[group, g], me, acr
        )

    turns = (2, 3, 1, 0)

    def step_over(group):
        rs_copy(group, 1).wait_recv()
        for g in turns:
            rows = slice(g * cap, (g + 1) * cap)
            rs_as[group, g] = (keep_v[group, 1, rows] + rs_r[group, 1, rows].astype(f32)).astype(
                bf16
            )
            rs_over(group, g).start()

    def ret_copy(block, peer, slot):
        return send(ret_s.at[block], ret_r.at[slot], ret_ss.at[block], ret_rs.at[slot], peer, t)

    def step_back(group):
        rs_copy(group, 0).wait_recv()
        for g in turns:
            span = slice(g * cap, (g + 1) * cap)
            part = keep_v[group, 0, span] + rs_r[group, 0, span].astype(f32)
            rs_over(group, g).wait_recv()
            rows = (part + rs_ar[group, g].astype(f32)).astype(bf16)
            src = groups[group][g]
            if group == 0 and g == 0:
                ret_r[src] = rows
            else:
                ret_s[src] = rows
                ret_copy(src, src, me).start()

    first_pass(groups[0], True)
    second_pass(groups[0])
    first_pass(groups[1], False)
    expert_share(0, groups[0])
    second_pass(groups[1])
    step_over(0)
    expert_share(1, groups[1])
    step_back(0)
    step_over(1)
    step_back(1)

    for d in range(1, n_sp):
        src = (me + d) % n_sp
        ret_copy(src, src, src).wait_recv()
    back = jnp.concatenate([ret_r[e].astype(f32) for e in range(n_sp)], axis=0).astype(bf16)
    taken0 = jnp.dot(pick0.astype(bf16), back, preferred_element_type=f32)
    taken1 = jnp.dot(pick1.astype(bf16), back, preferred_element_type=f32)
    routed = taken0 * by_token[:, 2:3] + taken1 * by_token[:, 3:4]
    out_ref[...] = (own_b.astype(f32) + routed).astype(bf16)

    for d in range(1, n_sp):
        peer = (me + d) % n_sp
        pack_copy(peer, peer, me).wait_send()
        send(att_s.at[peer], att_r.at[me], att_ss.at[peer], att_rs.at[me], peer, t).wait_send()
        disp_copy(peer, peer, me).wait_send()
        ret_copy(peer, peer, me).wait_send()
    mix_copy(0).wait_send()
    mix_copy(1).wait_send()
    mix_over.wait_send()
    for src in range(n_sp):
        pass_acr(src).wait_send()
        pass_sib(t, src, 0).wait_send()
        pass_sib(acr, src, 2).wait_send()
    for group in range(2):
        rs_copy(group, 0).wait_send()
        rs_copy(group, 1).wait_send()
        for g in range(quad):
            rs_over(group, g).wait_send()


def fused_device(n_sp, n_tp, *args):
    (
        residual,
        queries,
        keys,
        values,
        stick_bias,
        query_gain,
        key_gain,
        out_weight,
        norm_gain,
        route_ids,
        route_weights,
        gate_weight,
        up_weight,
        down_weight,
    ) = args
    tok, packed = queries.shape
    hd = query_gain.shape[0]
    model = residual.shape[1]
    own = model // n_tp
    hidden = gate_weight.shape[2]
    picks = route_ids.shape[1]
    cap = (5 * tok * picks + 4 * n_sp - 1) // (4 * n_sp)
    quad = n_sp // 2
    pairs = n_sp // 2
    half = tok // 2
    vmem = pl.BlockSpec(memory_space=pltpu.VMEM)
    anywhere = pl.BlockSpec(memory_space=pl.ANY)
    dma = pltpu.SemaphoreType.DMA
    scratch = [
        pltpu.VMEM((tok, own), bf16),
        pltpu.VMEM((packed, model), bf16),
        pltpu.VMEM((model, hidden), bf16),
        pltpu.VMEM((model, hidden), bf16),
        pltpu.VMEM((hidden, model), bf16),
        pltpu.VMEM((n_sp, tok + half + 16, 2 * hd), bf16),
        pltpu.VMEM((n_sp, tok + half + 16, 2 * hd), bf16),
        pltpu.VMEM((pairs, 2 * tok, hd), bf16),
        pltpu.VMEM((pairs, 2 * tok, hd), bf16),
        pltpu.VMEM((n_sp, half, 2 * hd), bf16),
        pltpu.VMEM((n_sp, half, 2 * hd), bf16),
        pltpu.VMEM((2, tok, own), bf16),
        pltpu.VMEM((2, tok, own), bf16),
        pltpu.VMEM((tok, own), bf16),
        pltpu.VMEM((tok, own), bf16),
        pltpu.VMEM((n_sp, cap, own), bf16),
        pltpu.VMEM((n_tp, n_sp, cap, own), bf16),
        pltpu.VMEM((quad * cap, model), bf16),
        pltpu.VMEM((2, 2, quad * cap, own), f32),
        pltpu.VMEM((2, 2, quad * cap, own), bf16),
        pltpu.VMEM((2, 2, quad * cap, own), bf16),
        pltpu.VMEM((2, quad, cap, own), bf16),
        pltpu.VMEM((2, quad, cap, own), bf16),
        pltpu.VMEM((n_sp, cap, own), bf16),
        pltpu.VMEM((n_sp, cap, own), bf16),
        dma((5,)),
        dma((n_sp,)),
        dma((n_sp,)),
        dma((n_sp,)),
        dma((n_sp,)),
        dma((3,)),
        dma((3,)),
        dma((n_sp,)),
        dma((n_tp, n_sp)),
        dma((3, n_sp)),
        dma((2, 2)),
        dma((2, 2)),
        dma((2, quad)),
        dma((2, quad)),
        dma((n_sp,)),
        dma((n_sp,)),
    ]
    return pl.pallas_call(
        functools.partial(fused_kernel, (n_sp, n_tp, tok, hd, cap, own)),
        out_shape=jax.ShapeDtypeStruct((tok, own), bf16),
        in_specs=[vmem] * 9 + [anywhere] * 5,
        out_specs=vmem,
        scratch_shapes=scratch,
        compiler_params=pltpu.CompilerParams(
            collective_id=0, has_side_effects=True, vmem_limit_bytes=56 * 1024 * 1024
        ),
    )(
        queries,
        keys,
        values,
        stick_bias,
        query_gain.reshape(1, -1),
        key_gain.reshape(1, -1),
        norm_gain.reshape(1, -1),
        route_ids.T,
        route_weights.T,
        residual,
        out_weight,
        gate_weight,
        up_weight,
        down_weight,
    )


def device_program(n_sp, n_tp, *args):
    tok, packed = args[1].shape
    hd = args[5].shape[0]
    picks = args[9].shape[1]
    cap = (5 * tok * picks + 4 * n_sp - 1) // (4 * n_sp)
    fits = (
        packed == n_sp * hd
        and tok == 2 * hd == 128
        and cap % 8 == 0
        and n_tp == 4
        and n_sp == 8
        and picks == 2
        and args[11].shape[0] == 1
    )
    if fits:
        return fused_device(n_sp, n_tp, *args)
    return per_device(*args)


def solution(mesh):
    placed = (
        P("sp", None),
        P("sp", "tp"),
        P("sp", "tp"),
        P("sp", "tp"),
        P("tp", "sp"),
        P(),
        P(),
        P("tp", None),
        P(),
        P("sp", None),
        P("sp", None),
        P("sp", None, "tp"),
        P("sp", None, "tp"),
        P("sp", "tp", None),
    )
    return jax.shard_map(
        functools.partial(device_program, mesh.shape["sp"], mesh.shape["tp"]),
        mesh=mesh, in_specs=placed, out_specs=P("sp", "tp"), check_vma=False
    )
```

```python
import functools
import math

import jax
import jax.numpy as jnp
from jax import lax
from jax.experimental import pallas as pl
from jax.experimental.pallas import tpu as pltpu
from jax.sharding import PartitionSpec as P

epsilon = 1e-06
clamp_limit = 7.0
swish_scale = 1.702


def head_normalize(packed, gain):
    values_f = packed.astype(jnp.float32).reshape(packed.shape[0], -1, gain.shape[0])
    scaled = (
        values_f * lax.rsqrt(jnp.mean(values_f * values_f, axis=-1, keepdims=True) + epsilon) * gain
    )
    return scaled.astype(jnp.bfloat16)


def activate(gate_pre, up_pre):
    gate_top = jnp.minimum(gate_pre, clamp_limit)
    up_clip = jnp.clip(up_pre, -clamp_limit, clamp_limit)
    return (up_clip + 1.0) * (gate_top * jax.nn.sigmoid(swish_scale * gate_top))


def slot_table(picked, expert_count, capacity):
    flat_ids = picked.reshape(-1)
    one_hot = (flat_ids[:, None] == jnp.arange(expert_count, dtype=jnp.int32)[None, :]).astype(
        jnp.int32
    )
    before = jnp.sum((jnp.cumsum(one_hot, axis=0) - one_hot) * one_hot, axis=1)
    return flat_ids * capacity + before


def key_block(state_pair, queries_n, keys_block, values_block, bias_block, first_key, query_pos):
    summed, log_carry = state_pair
    key_count = bias_block.shape[1]
    head_total = bias_block.shape[0]
    keys_heads = keys_block.reshape(key_count, head_total, -1)
    values_heads = values_block.reshape(key_count, head_total, -1)
    head_dim = keys_heads.shape[2]
    scores = jnp.einsum(
        "qhd,khd->hqk", queries_n, keys_heads, preferred_element_type=jnp.float32
    ) * head_dim ** (-0.5)
    scores = scores - bias_block.astype(jnp.float32)[:, None, :]
    key_pos = first_key + jnp.arange(key_count, dtype=jnp.int32)
    causal = ((key_pos[None, :] < query_pos[:, None]) & (key_pos[None, :] >= 0))[None]
    log_stay = jnp.where(causal, jax.nn.log_sigmoid(-scores), 0.0)
    later_sum = lax.cumsum(log_stay, axis=2, reverse=True) - log_stay
    weight = jnp.where(
        causal, jnp.exp(jax.nn.log_sigmoid(scores) + later_sum + log_carry[:, :, None]), 0.0
    )
    summed = summed + jnp.einsum(
        "hqk,khd->qhd",
        weight.astype(jnp.bfloat16),
        values_heads,
        preferred_element_type=jnp.float32,
    )
    return (summed, log_carry + jnp.sum(log_stay, axis=2))


def per_device(
    residual,
    queries,
    keys,
    values,
    stick_bias,
    query_gain,
    key_gain,
    out_weight,
    norm_gain,
    route_ids,
    route_weights,
    gate_weight,
    up_weight,
    down_weight,
):
    tok_rows = queries.shape[0]
    width_sp = lax.axis_size("sp")
    offset = lax.axis_index("sp") * tok_rows
    query_pos = offset + jnp.arange(tok_rows, dtype=jnp.int32)
    queries_n = head_normalize(queries, query_gain)
    keys_n = head_normalize(keys, key_gain).reshape(tok_rows, -1)
    head_total = stick_bias.shape[0]
    head_dim = query_gain.shape[0]
    state_pair = (
        jnp.zeros((tok_rows, head_total, head_dim), jnp.float32),
        jnp.zeros((head_total, tok_rows), jnp.float32),
    )
    all_keys, all_values, all_bias = (
        lax.all_gather(keys_n, "sp", axis=0, tiled=True),
        lax.all_gather(values, "sp", axis=0, tiled=True),
        lax.all_gather(stick_bias, "sp", axis=1, tiled=True),
    )
    key_total = all_keys.shape[0]
    block_len = math.gcd(key_total, 512)
    block_total = key_total // block_len

    def sweep_block(block_step, running):
        first_key = (block_total - 1 - block_step) * block_len
        return key_block(
            running,
            queries_n,
            lax.dynamic_slice_in_dim(all_keys, first_key, block_len, 0),
            lax.dynamic_slice_in_dim(all_values, first_key, block_len, 0),
            lax.dynamic_slice_in_dim(all_bias, first_key, block_len, 1),
            first_key,
            query_pos,
        )

    state_pair = lax.fori_loop(0, block_total, sweep_block, state_pair)
    attended = state_pair[0].reshape(tok_rows, head_total * head_dim).astype(jnp.bfloat16)
    partial_value = jnp.dot(attended, out_weight, preferred_element_type=jnp.float32)
    model_width = residual.shape[1]
    expert_count = width_sp * gate_weight.shape[0]
    pick_count = route_ids.shape[1]
    capacity = (5 * tok_rows * pick_count + 4 * expert_count - 1) // (4 * expert_count)
    slot_index = slot_table(route_ids, expert_count, capacity)
    assigned = slot_index.shape[0]
    source = (
        jnp.zeros((expert_count * capacity,), jnp.int32)
        .at[slot_index]
        .set(jnp.arange(assigned, dtype=jnp.int32) // pick_count)
    )
    filled = (
        jnp.zeros((expert_count * capacity,), jnp.bfloat16)
        .at[slot_index]
        .set(jnp.ones((assigned,), jnp.bfloat16))
    )
    gate_local = gate_weight[0]
    up_local = up_weight[0]
    down_local = down_weight[0]
    mixed_share = lax.psum_scatter(
        partial_value.astype(jnp.bfloat16), "tp", scatter_dimension=1, tiled=True
    ).astype(jnp.float32)
    own_width = mixed_share.shape[1]
    col_start = lax.axis_index("tp") * own_width
    own_res = lax.dynamic_slice_in_dim(residual, col_start, own_width, 1).astype(jnp.float32)
    own_cols = (own_res + mixed_share).astype(jnp.bfloat16).astype(jnp.float32)
    square_total = lax.psum(jnp.sum(own_cols * own_cols, axis=1), "tp")
    gain_cols = lax.dynamic_slice_in_dim(norm_gain, col_start, own_width, 0)
    normed_share = (
        own_cols * lax.rsqrt(square_total / model_width + epsilon)[:, None] * gain_cols
    ).astype(jnp.bfloat16)
    outgoing = (normed_share[source] * filled[:, None]).reshape(expert_count, capacity, -1)
    piece = lax.all_gather(
        lax.all_to_all(outgoing, "sp", split_axis=0, concat_axis=0, tiled=True),
        "tp",
        axis=2,
        tiled=True,
    )
    gate_pre = jnp.einsum("scd,df->scf", piece, gate_local, preferred_element_type=jnp.float32)
    up_pre = jnp.einsum("scd,df->scf", piece, up_local, preferred_element_type=jnp.float32)
    hidden = activate(gate_pre, up_pre).astype(jnp.bfloat16)
    share = jnp.einsum("scf,fd->scd", hidden, down_local, preferred_element_type=jnp.float32)
    returned = lax.psum_scatter(share.astype(jnp.bfloat16), "tp", scatter_dimension=2, tiled=True)
    arrived = lax.all_to_all(returned, "sp", split_axis=0, concat_axis=0, tiled=True)
    columns = arrived.shape[2]
    taken_rows = arrived.reshape(expert_count * capacity, columns)[slot_index]
    taken_rows = taken_rows.astype(jnp.float32).reshape(tok_rows, pick_count, columns)
    routed = jnp.sum(taken_rows * route_weights[:, :, None], axis=1)
    return (own_cols + routed).astype(jnp.bfloat16)


f32 = jnp.float32
bf16 = jnp.bfloat16
MESH = pl.DeviceIdType.MESH


def fused_kernel(
    dims,
    q_hbm,
    k_hbm,
    v_hbm,
    bias_hbm,
    qg_ref,
    kg_ref,
    ng_ref,
    ids_ref,
    rw_ref,
    res_hbm,
    ow_hbm,
    gw_hbm,
    uw_hbm,
    dw_hbm,
    out_ref,
    q_ref,
    k_ref,
    v_ref,
    bias_ref,
    qn_v,
    bias_v,
    sum_v,
    carry_v,
    res_v,
    ow_v,
    gw_v,
    uw_v,
    dw_v,
    pack_s,
    pack_r,
    kn_v,
    vn_v,
    att_s,
    att_r,
    mix_s,
    mix_r,
    mix_as,
    mix_ar,
    disp_s,
    x_v,
    z_v,
    keep_v,
    rs_s,
    rs_r,
    rs_as,
    rs_ar,
    ret_s,
    ret_r,
    w_sem,
    pack_ss,
    pack_rs,
    att_ss,
    att_rs,
    mix_ss,
    mix_rs,
    disp_ss,
    x_rs,
    fwd_ss,
    rs_ss,
    rs_rs,
    over_ss,
    over_rs,
    ret_ss,
    ret_rs,
):
    n_sp, n_tp, tok, hd, cap, own = dims
    me = lax.axis_index("sp")
    t = lax.axis_index("tp")
    sib = t + 1 - 2 * (t % 2)
    acr = (t + 2) % n_tp
    far = (sib + 2) % n_tp
    width = n_tp * own

    quad = n_sp // 2
    line = me // 2
    side = me % 2
    lines = [line, line + 1 - 2 * (line % 2), (line + 2) % quad, quad - 1 - line]
    groups = [[2 * at + side for at in lines], [2 * at + 1 - side for at in lines]]

    def send(src, dst, ss, rs, sp_id, tp_id):
        return pltpu.make_async_remote_copy(
            src_ref=src,
            dst_ref=dst,
            send_sem=ss,
            recv_sem=rs,
            device_id=(sp_id, tp_id),
            device_id_type=MESH,
        )

    def cols(index):
        return pl.ds(pl.multiple_of(index * own, own), own)

    loads = [
        pltpu.make_async_copy(ow_hbm, ow_v, w_sem.at[0]),
        pltpu.make_async_copy(res_hbm.at[:, cols(t)], res_v, w_sem.at[1]),
        pltpu.make_async_copy(gw_hbm.at[0], gw_v, w_sem.at[2]),
        pltpu.make_async_copy(uw_hbm.at[0], uw_v, w_sem.at[3]),
        pltpu.make_async_copy(dw_hbm.at[0], dw_v, w_sem.at[4]),
        pltpu.make_async_copy(q_hbm, q_ref, w_sem.at[5]),
        pltpu.make_async_copy(k_hbm, k_ref, w_sem.at[6]),
        pltpu.make_async_copy(v_hbm, v_ref, w_sem.at[7]),
        pltpu.make_async_copy(bias_hbm, bias_ref, w_sem.at[8]),
    ]
    barrier = pltpu.get_barrier_semaphore()
    for d in range(1, n_sp):
        pl.semaphore_signal(
            barrier, inc=1, device_id=((me + d) % n_sp, t), device_id_type=MESH
        )
    for peer in (sib, acr):
        pl.semaphore_signal(barrier, inc=1, device_id=(me, peer), device_id_type=MESH)

    for load in loads[5:] + loads[:5]:
        load.start()
    for load in loads[5:]:
        load.wait()

    half = tok // 2
    for h in range(n_sp):
        lanes = slice(h * hd, (h + 1) * hd)
        q_h = q_ref[:, lanes].astype(f32)
        k_h = k_ref[:, lanes].astype(f32)
        v_h = v_ref[:, lanes].astype(f32)
        pack_s[h, 0:tok, :] = jnp.concatenate([q_h, k_h], axis=1).astype(bf16)
        pack_s[h, tok : tok + half, :] = jnp.concatenate([v_h[:half], v_h[half:]], axis=1).astype(
            bf16
        )
        pack_s[h, tok + half : tok + half + 16, :] = jnp.broadcast_to(
            bias_ref[h : h + 1, :].astype(f32), (16, tok)
        ).astype(bf16)
    pl.semaphore_wait(barrier, n_sp + 1)

    def pack_copy(block, peer, slot):
        return send(
            pack_s.at[block], pack_r.at[slot], pack_ss.at[block], pack_rs.at[slot], peer, t
        )

    for peer in (
        [groups[0][1], groups[1][1], groups[1][0]] + groups[0][2:] + groups[1][2:]
    ):
        pack_copy(peer, peer, me).start()
    pack_r[me] = pack_s[me]

    by_token = jnp.transpose(
        jnp.concatenate(
            [ids_ref[...].astype(f32), rw_ref[...], jnp.zeros((4, tok), f32)], axis=0
        )
    )
    ids0 = by_token[:, 0:1]
    ids1 = by_token[:, 1:2]
    lane = lax.broadcasted_iota(jnp.int32, (tok, 128), 1).astype(f32)
    row = lax.broadcasted_iota(jnp.int32, (tok, tok), 0)
    col = lax.broadcasted_iota(jnp.int32, (tok, tok), 1)
    named0 = (lane == ids0).astype(f32)
    named1 = (lane == ids1).astype(f32)
    earlier = (col < row).astype(f32).astype(bf16)
    count = jnp.dot(earlier, (named0 + named1).astype(bf16), preferred_element_type=f32)
    slot0 = jnp.sum(named0 * count, axis=1, keepdims=True) + ids0 * cap
    slot1 = jnp.sum(named1 * count, axis=1, keepdims=True) + ids1 * cap
    slots = lax.broadcasted_iota(jnp.int32, (tok, n_sp * cap), 1).astype(f32)
    pick0 = (slots == slot0).astype(f32)
    pick1 = (slots == slot1).astype(f32)

    qb = 2 * tok
    row = lax.broadcasted_iota(jnp.int32, (qb, qb), 0)
    col = lax.broadcasted_iota(jnp.int32, (qb, qb), 1)
    causal = col < row
    tri = (row >= col).astype(f32).astype(bf16)

    def prepare(i):
        blocks = []
        v_blocks = []
        bias_i = []
        for b in (2 * i, 2 * i + 1):

            @pl.when(b != me)
            def _():
                pack_copy(b, b, b).wait_recv()

            blocks.append(pack_r[b, 0:tok, :].astype(f32))
            vp = pack_r[b, tok : tok + half, :].astype(f32)
            v_blocks += [vp[:, :hd], vp[:, hd:]]
            bias_i.append(pack_r[b, tok + half : tok + half + 16, :].astype(f32)[0:8])
        both = jnp.concatenate(blocks, axis=0)
        q_i = both[:, :hd]
        k_i = both[:, hd:]
        q_i = q_i * lax.rsqrt(jnp.mean(q_i * q_i, axis=1, keepdims=True) + epsilon) * qg_ref[...]
        k_i = k_i * lax.rsqrt(jnp.mean(k_i * k_i, axis=1, keepdims=True) + epsilon) * kg_ref[...]
        qn_v[i] = (q_i.astype(bf16).astype(f32) * hd**-0.5).astype(bf16)
        kn_v[i] = k_i.astype(bf16)
        vn_v[i] = jnp.concatenate(v_blocks, axis=0).astype(bf16)
        bias_v[i] = jnp.concatenate(bias_i, axis=1)

    def tile(i, j, state):
        s = lax.dot_general(
            qn_v[i], kn_v[j], (((1,), (1,)), ((), ())), preferred_element_type=f32
        )
        s = s - bias_v[j][0:1]
        leave = jnp.maximum(s, 0.0) + jnp.log(1.0 + jnp.exp(-jnp.abs(s)))
        if state is None:
            leave = jnp.where(causal, leave, 0.0)
        top = leave.astype(bf16)
        low = (leave - top.astype(f32)).astype(bf16)
        total = jnp.dot(top, tri, preferred_element_type=f32) + jnp.dot(
            low, tri, preferred_element_type=f32
        )
        if state is None:
            weight = jnp.where(causal, jnp.exp(s - total), 0.0)
        else:
            weight = jnp.exp(s - total - state[1])
        part = jnp.dot(weight.astype(bf16), vn_v[j], preferred_element_type=f32)
        if state is None:
            return part, total[:, 0:1]
        return state[0] + part, state[1] + total[:, 0:1]

    def give_back(i, summed):
        for r in range(2):
            b = 2 * i + r
            part = summed[r * tok : (r + 1) * tok]
            packed = jnp.concatenate([part[:half], part[half:]], axis=1).astype(bf16)
            att_s[b] = packed

            @pl.when(b != me)
            def _():
                send(att_s.at[b], att_r.at[me], att_ss.at[b], att_rs.at[me], b, t).start()

            @pl.when(b == me)
            def _():
                att_r[b] = packed

    def triangle(half_id):
        first = half_id * (quad // 2)
        prepare(first)
        prepare(first + 1)
        state0 = tile(first, first, None)
        state1 = tile(first + 1, first, tile(first + 1, first + 1, None))
        for i, state in ((first, state0), (first + 1, state1)):
            sum_v[i] = state[0]
            carry_v[i] = jnp.broadcast_to(state[1], (qb, 128))

    near_half = line // (quad // 2)
    triangle(near_half)

    @pl.when(near_half == 0)
    def _():
        for i in range(2):
            give_back(i, sum_v[i])

    triangle(1 - near_half)

    @pl.when(near_half == 1)
    def _():
        for i in range(2):
            give_back(i, sum_v[i])

    for i in (2, 3):
        state = (sum_v[i], carry_v[i][:, 0:1])
        for j in (1, 0):
            state = tile(i, j, state)
        give_back(i, state[0])

    for h in range(n_sp):

        @pl.when(h != me)
        def _():
            send(att_s.at[h], att_r.at[h], att_ss.at[h], att_rs.at[h], h, t).wait_recv()

    heads = []
    for h in range(n_sp):
        p = att_r[h].astype(f32)
        heads.append(jnp.concatenate([p[:, :hd], p[:, hd:]], axis=0))
    attended = jnp.concatenate(heads, axis=1).astype(bf16)

    loads[0].wait()

    def project(index):
        return jnp.dot(attended, ow_v[:, cols(index)], preferred_element_type=f32)

    def mix_copy(slot):
        return send(mix_s.at[slot], mix_r.at[slot], mix_ss.at[slot], mix_rs.at[slot], me, sib)

    mix_s[1] = project(far).astype(bf16)
    mix_copy(1).start()
    mix_s[0] = project(sib).astype(bf16)
    mix_copy(0).start()
    across = project(acr)
    mix_copy(1).wait_recv()
    mix_as[...] = (across + mix_r[1].astype(f32)).astype(bf16)
    mix_over = send(mix_as, mix_ar, mix_ss.at[2], mix_rs.at[2], me, acr)
    mix_over.start()
    mixed = project(t)
    loads[1].wait()
    mix_copy(0).wait_recv()
    mixed = mixed + mix_r[0].astype(f32) + res_v[...].astype(f32)
    mix_over.wait_recv()
    own_b = (mixed + mix_ar[...].astype(f32)).astype(bf16)

    spread = lax.dot_general(
        (pick0 + pick1).astype(bf16), own_b, (((0,), (0,)), ((), ())), preferred_element_type=f32
    )
    for e in range(n_sp):
        disp_s[e] = spread[e * cap : (e + 1) * cap].astype(bf16)

    def disp_copy(block, peer, slot):
        return send(
            disp_s.at[block], x_v.at[t, slot], disp_ss.at[block], x_rs.at[t, slot], peer, t
        )

    for peer in groups[0][1:] + groups[1]:
        disp_copy(peer, peer, me).start()
    x_v[t, me] = disp_s[me]

    def pass_sib(column, src, sem):
        return send(
            x_v.at[column, src],
            x_v.at[column, src],
            fwd_ss.at[sem, src],
            x_rs.at[column, src],
            me,
            sib,
        )

    def pass_acr(src):
        return send(x_v.at[t, src], x_v.at[t, src], fwd_ss.at[1, src], x_rs.at[t, src], me, acr)

    def came(column, src):
        send(
            x_v.at[column, src], x_v.at[column, src], fwd_ss.at[0, src], x_rs.at[column, src], me, sib
        ).wait_recv()

    def first_pass(srcs, skip_first):
        for g, src in enumerate(srcs):
            if not (skip_first and g == 0):
                came(t, src)
            pass_acr(src).start()
            pass_sib(t, src, 0).start()

    def second_pass(srcs):
        for src in srcs:
            came(acr, src)
            pass_sib(acr, src, 2).start()

    def expert_share(group, srcs):
        for src in srcs:
            came(sib, src)
            came(far, src)
        pieces = []
        for src in srcs:
            pieces.append(jnp.concatenate([x_v[c, src].astype(f32) for c in range(n_tp)], axis=1))
        rows = jnp.concatenate(pieces, axis=0)
        scale = lax.rsqrt(jnp.mean(rows * rows, axis=1, keepdims=True) + epsilon)
        z_v[...] = (rows * scale * ng_ref[...]).astype(bf16)
        if group == 0:
            loads[2].wait()
            loads[3].wait()
        gate_pre = jnp.dot(z_v[...], gw_v[...], preferred_element_type=f32)
        up_pre = jnp.dot(z_v[...], uw_v[...], preferred_element_type=f32)
        hidden = activate(gate_pre, up_pre).astype(bf16)
        if group == 0:
            loads[4].wait()

        def down(index):
            return jnp.dot(hidden, dw_v[:, cols(index)], preferred_element_type=f32)

        rs_s[group, 1] = down(far).astype(bf16)
        rs_copy(group, 1).start()
        rs_s[group, 0] = down(sib).astype(bf16)
        rs_copy(group, 0).start()
        keep_v[group, 1] = down(acr)
        keep_v[group, 0] = down(t)

    def rs_copy(group, slot):
        return send(
            rs_s.at[group, slot],
            rs_r.at[group, slot],
            rs_ss.at[group, slot],
            rs_rs.at[group, slot],
            me,
            sib,
        )

    def rs_over(group, g):
        return send(
            rs_as.at[group, g], rs_ar.at[group, g], over_ss.at[group, g], over_rs.at[group, g], me, acr
        )

    turns = (2, 3, 1, 0)

    def step_over(group):
        rs_copy(group, 1).wait_recv()
        for g in turns:
            rows = slice(g * cap, (g + 1) * cap)
            rs_as[group, g] = (keep_v[group, 1, rows] + rs_r[group, 1, rows].astype(f32)).astype(
                bf16
            )
            rs_over(group, g).start()

    def ret_copy(block, peer, slot):
        return send(ret_s.at[block], ret_r.at[slot], ret_ss.at[block], ret_rs.at[slot], peer, t)

    def step_back(group):
        rs_copy(group, 0).wait_recv()
        for g in turns:
            span = slice(g * cap, (g + 1) * cap)
            part = keep_v[group, 0, span] + rs_r[group, 0, span].astype(f32)
            rs_over(group, g).wait_recv()
            rows = (part + rs_ar[group, g].astype(f32)).astype(bf16)
            src = groups[group][g]
            if group == 0 and g == 0:
                ret_r[src] = rows
            else:
                ret_s[src] = rows
                ret_copy(src, src, me).start()

    first_pass(groups[0], True)
    second_pass(groups[0])
    first_pass(groups[1], False)
    expert_share(0, groups[0])
    second_pass(groups[1])
    step_over(0)
    expert_share(1, groups[1])
    step_over(1)
    step_back(0)
    step_back(1)

    for d in range(1, n_sp):
        src = (me + d) % n_sp
        ret_copy(src, src, src).wait_recv()
    back = jnp.concatenate([ret_r[e].astype(f32) for e in range(n_sp)], axis=0).astype(bf16)
    taken0 = jnp.dot(pick0.astype(bf16), back, preferred_element_type=f32)
    taken1 = jnp.dot(pick1.astype(bf16), back, preferred_element_type=f32)
    routed = taken0 * by_token[:, 2:3] + taken1 * by_token[:, 3:4]
    out_ref[...] = (own_b.astype(f32) + routed).astype(bf16)

    for d in range(1, n_sp):
        peer = (me + d) % n_sp
        pack_copy(peer, peer, me).wait_send()
        send(att_s.at[peer], att_r.at[me], att_ss.at[peer], att_rs.at[me], peer, t).wait_send()
        disp_copy(peer, peer, me).wait_send()
        ret_copy(peer, peer, me).wait_send()
    mix_copy(0).wait_send()
    mix_copy(1).wait_send()
    mix_over.wait_send()
    for src in range(n_sp):
        pass_acr(src).wait_send()
        pass_sib(t, src, 0).wait_send()
        pass_sib(acr, src, 2).wait_send()
    for group in range(2):
        rs_copy(group, 0).wait_send()
        rs_copy(group, 1).wait_send()
        for g in range(quad):
            rs_over(group, g).wait_send()


def fused_device(n_sp, n_tp, *args):
    (
        residual,
        queries,
        keys,
        values,
        stick_bias,
        query_gain,
        key_gain,
        out_weight,
        norm_gain,
        route_ids,
        route_weights,
        gate_weight,
        up_weight,
        down_weight,
    ) = args
    tok, packed = queries.shape
    hd = query_gain.shape[0]
    model = residual.shape[1]
    own = model // n_tp
    hidden = gate_weight.shape[2]
    picks = route_ids.shape[1]
    cap = (5 * tok * picks + 4 * n_sp - 1) // (4 * n_sp)
    quad = n_sp // 2
    pairs = n_sp // 2
    half = tok // 2
    vmem = pl.BlockSpec(memory_space=pltpu.VMEM)
    anywhere = pl.BlockSpec(memory_space=pl.ANY)
    dma = pltpu.SemaphoreType.DMA
    scratch = [
        pltpu.VMEM((tok, packed), bf16),
        pltpu.VMEM((tok, packed), bf16),
        pltpu.VMEM((tok, packed), bf16),
        pltpu.VMEM((n_sp, tok), bf16),
        pltpu.VMEM((pairs, 2 * tok, hd), bf16),
        pltpu.VMEM((pairs, 8, 2 * tok), f32),
        pltpu.VMEM((pairs, 2 * tok, hd), f32),
        pltpu.VMEM((pairs, 2 * tok, 128), f32),
        pltpu.VMEM((tok, own), bf16),
        pltpu.VMEM((packed, model), bf16),
        pltpu.VMEM((model, hidden), bf16),
        pltpu.VMEM((model, hidden), bf16),
        pltpu.VMEM((hidden, model), bf16),
        pltpu.VMEM((n_sp, tok + half + 16, 2 * hd), bf16),
        pltpu.VMEM((n_sp, tok + half + 16, 2 * hd), bf16),
        pltpu.VMEM((pairs, 2 * tok, hd), bf16),
        pltpu.VMEM((pairs, 2 * tok, hd), bf16),
        pltpu.VMEM((n_sp, half, 2 * hd), bf16),
        pltpu.VMEM((n_sp, half, 2 * hd), bf16),
        pltpu.VMEM((2, tok, own), bf16),
        pltpu.VMEM((2, tok, own), bf16),
        pltpu.VMEM((tok, own), bf16),
        pltpu.VMEM((tok, own), bf16),
        pltpu.VMEM((n_sp, cap, own), bf16),
        pltpu.VMEM((n_tp, n_sp, cap, own), bf16),
        pltpu.VMEM((quad * cap, model), bf16),
        pltpu.VMEM((2, 2, quad * cap, own), f32),
        pltpu.VMEM((2, 2, quad * cap, own), bf16),
        pltpu.VMEM((2, 2, quad * cap, own), bf16),
        pltpu.VMEM((2, quad, cap, own), bf16),
        pltpu.VMEM((2, quad, cap, own), bf16),
        pltpu.VMEM((n_sp, cap, own), bf16),
        pltpu.VMEM((n_sp, cap, own), bf16),
        dma((9,)),
        dma((n_sp,)),
        dma((n_sp,)),
        dma((n_sp,)),
        dma((n_sp,)),
        dma((3,)),
        dma((3,)),
        dma((n_sp,)),
        dma((n_tp, n_sp)),
        dma((3, n_sp)),
        dma((2, 2)),
        dma((2, 2)),
        dma((2, quad)),
        dma((2, quad)),
        dma((n_sp,)),
        dma((n_sp,)),
    ]
    return pl.pallas_call(
        functools.partial(fused_kernel, (n_sp, n_tp, tok, hd, cap, own)),
        out_shape=jax.ShapeDtypeStruct((tok, own), bf16),
        in_specs=[anywhere] * 4 + [vmem] * 5 + [anywhere] * 5,
        out_specs=vmem,
        scratch_shapes=scratch,
        compiler_params=pltpu.CompilerParams(
            collective_id=0, has_side_effects=True, vmem_limit_bytes=63 * 1024 * 1024
        ),
    )(
        queries,
        keys,
        values,
        stick_bias,
        query_gain.reshape(1, -1),
        key_gain.reshape(1, -1),
        norm_gain.reshape(1, -1),
        route_ids.T,
        route_weights.T,
        residual,
        out_weight,
        gate_weight,
        up_weight,
        down_weight,
    )


def device_program(n_sp, n_tp, *args):
    tok, packed = args[1].shape
    hd = args[5].shape[0]
    picks = args[9].shape[1]
    cap = (5 * tok * picks + 4 * n_sp - 1) // (4 * n_sp)
    fits = (
        packed == n_sp * hd
        and tok == 2 * hd == 128
        and cap % 8 == 0
        and n_tp == 4
        and n_sp == 8
        and picks == 2
        and args[11].shape[0] == 1
    )
    if fits:
        return fused_device(n_sp, n_tp, *args)
    return per_device(*args)


def solution(mesh):
    placed = (
        P("sp", None),
        P("sp", "tp"),
        P("sp", "tp"),
        P("sp", "tp"),
        P("tp", "sp"),
        P(),
        P(),
        P("tp", None),
        P(),
        P("sp", None),
        P("sp", None),
        P("sp", None, "tp"),
        P("sp", None, "tp"),
        P("sp", "tp", None),
    )
    return jax.shard_map(
        functools.partial(device_program, mesh.shape["sp"], mesh.shape["tp"]),
        mesh=mesh, in_specs=placed, out_specs=P("sp", "tp"), check_vma=False
    )
```
